32 devices in a mesh: sp: 32 (over z, y, x, core), tp: 1.
Axes of the slice: x: 2, y: 2, z: 4, core: 2. Of those that a mesh axis runs over, the one named last changes fastest.
Arguments:
- stream: bfloat16 [8192, 2048], P(('sp', 'tp')), may hold values from -6 to 6
- query_one: bfloat16 [8192, 512], P('sp', 'tp'), may hold values from -280 to 280
- key_one: bfloat16 [8192, 512], P('sp', 'tp'), may hold values from -6 to 6
- query_two: bfloat16 [8192, 512], P('sp', 'tp'), may hold values from -280 to 280
- key_two: bfloat16 [8192, 512], P('sp', 'tp'), may hold values from -6 to 6
- values: bfloat16 [8192, 1024], P('sp', 'tp'), may hold values from -6 to 6
- lambdas: float32 [8], P('tp'), may hold values from 0.3 to 0.8
- head_gain: float32 [128], replicated, may hold values from 0.1 to 1.9
- out_weight: bfloat16 [1024, 2048], replicated, may hold values from -0.1875 to 0.1875
- norm_gain: float32 [2048], replicated, may hold values from 0.1 to 1.9
- gate_weight: bfloat16 [2048, 2816], P('sp', 'tp'), may hold values from -0.125 to 0.125
- up_weight: bfloat16 [2048, 2816], P('sp', 'tp'), may hold values from -0.125 to 0.125
- down_weight: bfloat16 [2816, 2048], P('tp', 'sp'), may hold values from -0.3125 to 0.3125
Outputs:
- result: bfloat16 [8192, 2048], P(('sp', 'tp'))
The draws below stay inside these ranges and needn't reach their ends.
All inputs are finite; a program needn't handle non-finite values.
Results may differ from the reference program's by a relative error of at most 0.014.
Values may be sent and summed in bfloat16 or wider, within the bound.
A program may use at most 192 MiB of HBM per device.

```python
import jax
import jax.numpy as jnp
from jax import lax

D = 2048
HEADS = 8
HEAD_DIM = 64
VDIM = 128
FF = 2816
SEQ = 8192
N_TP = 1


def drawn_pair(key, tag):
    folded = jax.random.fold_in(key, tag)
    query_seed, key_seed = jax.random.split(folded)
    row_width = HEADS * HEAD_DIM
    queries = jnp.clip(jax.random.normal(query_seed, (SEQ, row_width), jnp.float32), -6.0, 6.0) * 1.75
    keys = jnp.clip(jax.random.normal(key_seed, (SEQ, row_width), jnp.float32), -6.0, 6.0)
    return (queries, keys)


def draw_query_one(key, part):
    return drawn_pair(key, 11)[0].astype(jnp.bfloat16)


def draw_key_one(key, part):
    return drawn_pair(key, 11)[1].astype(jnp.bfloat16)


def draw_query_two(key, part):
    return drawn_pair(key, 23)[0].astype(jnp.bfloat16)


def draw_key_two(key, part):
    return drawn_pair(key, 23)[1].astype(jnp.bfloat16)


def block_scale(key, extent, pieces, least, largest):
    factor_of, own = 1.0, jax.random.fold_in(key, 6)
    for axis_at, blocks in pieces:
        steps = jnp.exp(jax.random.uniform(jax.random.fold_in(own, axis_at), (blocks,), jnp.float32, least / len(pieces), largest / len(pieces)))
        factor_of = factor_of * jnp.repeat(steps, extent[axis_at] // blocks).reshape([-1 if axis == axis_at else 1 for axis in range(len(extent))])
    return factor_of


def noise(key, extent, width, bound, cuts=(), kind=jnp.bfloat16):
    values = width * jax.random.normal(key, extent, jnp.float32)
    if cuts:
        values = values * block_scale(key, extent, cuts, -0.22, 0.18)
    return jnp.clip(values, -bound, bound).astype(kind)


def setup_inputs(seed: int = 0) -> dict:
    key_of = jax.random.split(jax.random.key(seed), 14)
    return {
        "stream": noise(key_of[0], (SEQ, D), 1.0, 6.0, ((0, 32),)),
        "query_one": draw_query_one(jax.random.fold_in(key_of[13], 71), 0),
        "key_one": draw_key_one(jax.random.fold_in(key_of[13], 71), 0),
        "query_two": draw_query_two(jax.random.fold_in(key_of[13], 71), 0),
        "key_two": draw_key_two(jax.random.fold_in(key_of[13], 71), 0),
        "values": noise(key_of[5], (SEQ, HEADS * VDIM), 1.0, 6.0, ((0, 32),)),
        "lambdas": jnp.clip(jax.random.uniform(key_of[6], (HEADS,), jnp.float32, 0.3, 0.8), 0.3, 0.8),
        "head_gain": jnp.clip(1.0 + 0.18 * jax.random.normal(key_of[7], (VDIM,), jnp.float32), 0.1, 1.9),
        "out_weight": noise(key_of[8], (HEADS * VDIM, D), (HEADS * VDIM) ** -0.5, 0.1875),
        "norm_gain": jnp.clip(1.0 + 0.18 * jax.random.normal(key_of[9], (D,), jnp.float32), 0.1, 1.9),
        "gate_weight": noise(key_of[10], (D, FF), D ** -0.5, 0.125, ((0, 32),)),
        "up_weight": noise(key_of[11], (D, FF), D ** -0.5, 0.125, ((0, 32),)),
        "down_weight": noise(key_of[12], (FF, D), (FF // 9) ** -0.5, 0.3125, ((1, 32),)),
    }


ALPHA = 1.4142135623730951
EPSILON = 1e-05

def one_map(queries, keys, value_rows):
    factor = HEAD_DIM ** (-0.5)
    scores = jnp.einsum('qhd,khd->hqk', queries.astype(jnp.float32), keys.astype(jnp.float32)) * factor
    row_peak = lax.optimization_barrier(jnp.max(scores, axis=-1, keepdims=True))
    weights = jnp.exp(scores - row_peak)
    totals = lax.optimization_barrier(jnp.sum(weights, axis=-1))
    rounded = lax.optimization_barrier(weights.astype(jnp.bfloat16))
    summed = jnp.einsum('hqk,khe->qhe', rounded.astype(jnp.float32), value_rows.astype(jnp.float32))
    return summed / jnp.transpose(totals)[:, :, None]

def layer_normed(heads_rows, residual_rows, out_weight, norm_gain):
    branch = jnp.dot(heads_rows, out_weight, preferred_element_type=jnp.float32)
    mixed_in = ALPHA * residual_rows.astype(jnp.float32) + branch
    row_mean = lax.optimization_barrier(jnp.mean(mixed_in, axis=-1, keepdims=True))
    centered = mixed_in - row_mean
    row_var = lax.optimization_barrier(jnp.mean(centered * centered, axis=-1, keepdims=True))
    return (centered * lax.rsqrt(row_var + EPSILON) * norm_gain).astype(jnp.bfloat16)

def reference(stream, query_one, key_one, query_two, key_two, values, lambdas, head_gain, out_weight, norm_gain, gate_weight, up_weight, down_weight):
    keys_first = key_one.reshape(SEQ, HEADS, HEAD_DIM)
    keys_second = key_two.reshape(SEQ, HEADS, HEAD_DIM)
    value_rows = values.reshape(SEQ, HEADS, VDIM)
    block_rows = 256
    block_count = SEQ // block_rows

    def attend(position):
        begin_row = position * block_rows
        first_rows = lax.dynamic_slice_in_dim(query_one, begin_row, block_rows, 0).reshape(block_rows, HEADS, HEAD_DIM)
        second_rows = lax.dynamic_slice_in_dim(query_two, begin_row, block_rows, 0).reshape(block_rows, HEADS, HEAD_DIM)
        first_map = one_map(first_rows, keys_first, value_rows)
        second = one_map(second_rows, keys_second, value_rows)
        differ = first_map - lambdas[None, :, None] * second
        inverse_rms = lax.rsqrt(lax.optimization_barrier(jnp.mean(differ * differ, axis=-1, keepdims=True)) + EPSILON)
        return (differ * inverse_rms * head_gain * 0.8).astype(jnp.bfloat16).reshape(block_rows, HEADS * VDIM)
    attended = lax.map(attend, jnp.arange(block_count, dtype=jnp.int32)).reshape(SEQ, HEADS * VDIM)
    normed = layer_normed(attended, stream, out_weight, norm_gain)
    gate_out = jnp.dot(normed, gate_weight, preferred_element_type=jnp.float32)
    upward = jnp.dot(normed, up_weight, preferred_element_type=jnp.float32)
    hidden = (jax.nn.silu(gate_out) * upward).astype(jnp.bfloat16)
    group_width = FF // N_TP
    mixer_out = jnp.zeros((SEQ, D), jnp.float32)
    for group_index in range(N_TP):
        low_unit = group_index * group_width
        partial_value = jnp.dot(hidden[:, low_unit:low_unit + group_width], down_weight[low_unit:low_unit + group_width, :], preferred_element_type=jnp.float32)
        partial_value = lax.optimization_barrier(partial_value.astype(jnp.bfloat16))
        mixer_out = mixer_out + partial_value.astype(jnp.float32)
    return (ALPHA * normed.astype(jnp.float32) + 0.5 * mixer_out).astype(jnp.bfloat16)
```

```python
import functools

import jax
import jax.numpy as jnp
from jax import lax
from jax.experimental import pallas as pl
from jax.experimental.pallas import tpu as pltpu
from jax.sharding import PartitionSpec as P

ALPHA = 1.4142135623730951
EPSILON = 1e-05


def attend_kernel(first, last, factor, block_keys, *refs):
    refs = list(refs)
    lam_ref, gain_ref, q_ref, kv_ref = refs[:4]
    refs = refs[4:]
    if not first:
        m_in, acc_in = refs[:2]
        refs = refs[2:]
    if last:
        (out_ref,) = refs[:1]
        refs = refs[1:]
    else:
        m_out, acc_out = refs[:2]
        refs = refs[2:]
    (vext,) = refs
    rows, width = q_ref.shape
    head = width // 2
    keys = kv_ref.shape[0]
    vdim = kv_ref.shape[1] - width

    @pl.when(pl.program_id(0) == 0)
    def _():
        vext[:, :vdim] = kv_ref[:, width:]
        vext[:, vdim:] = jnp.ones((keys, vdim), vext.dtype)

    q = q_ref[...] * jnp.asarray(factor, q_ref.dtype)
    lane = lax.broadcasted_iota(jnp.int32, q.shape, 1)
    zero = jnp.zeros_like(q)
    maps = [jnp.where(lane < head, q, zero), jnp.where(lane < head, zero, q)]
    ms, accs = [], []
    for i in range(2):
        if first:
            ms.append(jnp.full((rows, 1), -1e30, jnp.float32))
            accs.append(None)
        else:
            ms.append(m_in[i][:, :1])
            accs.append(acc_in[i])
    for start in range(0, keys, block_keys):
        kk = kv_ref[start : start + block_keys, :width]
        vv = vext[start : start + block_keys, :]
        for i in range(2):
            s = lax.dot_general(maps[i], kk, (((1,), (1,)), ((), ())), preferred_element_type=jnp.float32)
            m_new = jnp.maximum(ms[i], jnp.max(s, axis=1, keepdims=True))
            p = jnp.exp(s - m_new).astype(jnp.bfloat16)
            pv = jnp.dot(p, vv, preferred_element_type=jnp.float32)
            if accs[i] is None:
                accs[i] = pv
            else:
                accs[i] = accs[i] * jnp.exp(ms[i] - m_new) + pv
            ms[i] = m_new
    if last:
        o = [a[:, :vdim] / a[:, vdim:] for a in accs]
        differ = o[0] - lam_ref[0] * o[1]
        inverse = lax.rsqrt(jnp.mean(differ * differ, axis=1, keepdims=True) + EPSILON)
        out_ref[...] = (differ * inverse * gain_ref[...] * 0.8).astype(out_ref.dtype)
    else:
        for i in range(2):
            m_out[i] = jnp.broadcast_to(ms[i], (rows, m_out.shape[2]))
            acc_out[i] = accs[i]


def attend(lam, gain, q, kv, state, last, factor):
    rows, width = q.shape
    keys = kv.shape[0]
    vdim = kv.shape[1] - width
    block = min(256, rows)
    first = state is None
    smem = pl.BlockSpec(memory_space=pltpu.SMEM)
    m_spec = pl.BlockSpec((2, block, 128), lambda i: (0, i, 0))
    acc_spec = pl.BlockSpec((2, block, 2 * vdim), lambda i: (0, i, 0))
    in_specs = [
        smem,
        pl.BlockSpec((1, vdim), lambda i: (0, 0)),
        pl.BlockSpec((block, width), lambda i: (i, 0)),
        pl.BlockSpec((keys, width + vdim), lambda i: (0, 0)),
    ]
    args = [lam, gain, q, kv]
    aliases = {}
    if not first:
        in_specs += [m_spec, acc_spec]
        args += list(state)
        if not last:
            aliases = {4: 0, 5: 1}
    if last:
        out_shape = jax.ShapeDtypeStruct((rows, vdim), jnp.bfloat16)
        out_specs = pl.BlockSpec((block, vdim), lambda i: (i, 0))
    else:
        out_shape = (
            jax.ShapeDtypeStruct((2, rows, 128), jnp.float32),
            jax.ShapeDtypeStruct((2, rows, 2 * vdim), jnp.float32),
        )
        out_specs = (m_spec, acc_spec)
    return pl.pallas_call(
        functools.partial(attend_kernel, first, last, factor, min(1024, keys)),
        grid=(rows // block,),
        in_specs=in_specs,
        out_specs=out_specs,
        out_shape=out_shape,
        input_output_aliases=aliases,
        scratch_shapes=[pltpu.VMEM((keys, 2 * vdim), jnp.bfloat16)],
        compiler_params=pltpu.CompilerParams(dimension_semantics=("arbitrary",)),
    )(*args)


def layer_normed(heads_rows, residual_rows, out_weight, norm_gain):
    branch = jnp.dot(heads_rows, out_weight, preferred_element_type=jnp.float32)
    mixed_in = ALPHA * residual_rows.astype(jnp.float32) + branch
    row_mean = jnp.mean(mixed_in, axis=-1, keepdims=True)
    centered = mixed_in - row_mean
    row_var = jnp.mean(centered * centered, axis=-1, keepdims=True)
    return (centered * lax.rsqrt(row_var + EPSILON) * norm_gain).astype(jnp.bfloat16)


def on_device(
    stream,
    query_one,
    key_one,
    query_two,
    key_two,
    values,
    lambdas,
    head_gain,
    out_weight,
    norm_gain,
    gate_weight,
    up_weight,
    down_weight,
):
    heads = lambdas.shape[0]
    tokens = query_one.shape[0]
    head_width = query_one.shape[1] // heads
    vdim = values.shape[1] // heads
    hidden_units = gate_weight.shape[1]
    group = lax.axis_size("sp")
    tp = lax.axis_size("tp")
    ring = group // heads
    me = lax.axis_index("sp")
    factor = head_width ** (-0.5)

    packed = jnp.concatenate([gate_weight, up_weight, down_weight.T], axis=1)
    weights = lax.all_gather(packed, "sp", axis=0, tiled=True)

    def by_head(a):
        return jnp.transpose(a.reshape(tokens, heads, a.shape[1] // heads), (1, 0, 2))

    own = jnp.concatenate([by_head(a) for a in (query_one, query_two, key_one, key_two, values)], axis=2)
    near = [[r * heads + h for h in range(heads)] for r in range(ring)]
    mine = lax.all_to_all(own, "sp", split_axis=0, concat_axis=0, axis_index_groups=near, tiled=True)
    mine = mine.reshape(heads * tokens, own.shape[2])
    q = mine[:, : 2 * head_width]
    kv = mine[:, 2 * head_width :]
    lam = lax.dynamic_slice_in_dim(lambdas, lax.rem(me, heads), 1, 0)
    gain = head_gain.reshape(1, vdim)
    onward = [(d, (d + heads) % group) for d in range(group)]
    state = None
    for step in range(ring):
        following = lax.ppermute(kv, "sp", onward) if step + 1 < ring else None
        state = attend(lam, gain, q, kv, state, step + 1 == ring, factor)
        kv = following
    back = lax.all_to_all(
        state.reshape(heads, tokens, vdim), "sp", split_axis=0, concat_axis=0, axis_index_groups=near, tiled=True
    )
    attended = jnp.transpose(back, (1, 0, 2)).reshape(tokens, heads * vdim)

    by_rows = lax.all_to_all(attended, "tp", split_axis=0, concat_axis=1, tiled=True) if tp > 1 else attended
    own_normed = layer_normed(by_rows, stream, out_weight, norm_gain)
    normed_all = lax.all_gather(own_normed, "tp", axis=0, tiled=True) if tp > 1 else own_normed
    gate_out = jnp.dot(normed_all, weights[:, :hidden_units], preferred_element_type=jnp.float32)
    upward = jnp.dot(normed_all, weights[:, hidden_units : 2 * hidden_units], preferred_element_type=jnp.float32)
    hidden = (jax.nn.silu(gate_out) * upward).astype(jnp.bfloat16)
    partial_terms = lax.dot_general(
        hidden, weights[:, 2 * hidden_units :], (((1,), (1,)), ((), ())), preferred_element_type=jnp.float32
    ).astype(jnp.bfloat16)
    if tp > 1:
        partial_terms = lax.psum_scatter(partial_terms, "tp", scatter_dimension=0, tiled=True)
    mixer_out = partial_terms.astype(jnp.float32)
    return (ALPHA * own_normed.astype(jnp.float32) + 0.5 * mixer_out).astype(jnp.bfloat16)


def solution(mesh):
    return jax.shard_map(
        on_device,
        mesh=mesh,
        in_specs=(
            P(("sp", "tp"), None),
            P("sp", "tp"),
            P("sp", "tp"),
            P("sp", "tp"),
            P("sp", "tp"),
            P("sp", "tp"),
            P("tp"),
            P(),
            P(),
            P(),
            P("sp", "tp"),
            P("sp", "tp"),
            P("tp", "sp"),
        ),
        out_specs=P(("sp", "tp"), None),
        check_vma=False,
    )
```

```python
import functools

import jax
import jax.numpy as jnp
from jax import lax
from jax.experimental import pallas as pl
from jax.experimental.pallas import tpu as pltpu
from jax.sharding import PartitionSpec as P

ALPHA = 1.4142135623730951
EPSILON = 1e-05


def attend_kernel(first, last, factor, block_keys, *refs):
    refs = list(refs)
    lam_ref, gain_ref, q_ref, kv_ref = refs[:4]
    refs = refs[4:]
    if not first:
        m_in, acc_in = refs[:2]
        refs = refs[2:]
    if last:
        (out_ref,) = refs[:1]
        refs = refs[1:]
    else:
        m_out, acc_out = refs[:2]
        refs = refs[2:]
    (vext,) = refs
    rows, width = q_ref.shape
    head = width // 2
    keys = kv_ref.shape[0]
    vdim = kv_ref.shape[1] - width

    @pl.when(pl.program_id(0) == 0)
    def _():
        vext[:, :vdim] = kv_ref[:, width:]
        vext[:, vdim:] = jnp.ones((keys, vdim), vext.dtype)

    q = q_ref[...] * jnp.asarray(factor, q_ref.dtype)
    lane = lax.broadcasted_iota(jnp.int32, q.shape, 1)
    zero = jnp.zeros_like(q)
    maps = [jnp.where(lane < head, q, zero), jnp.where(lane < head, zero, q)]
    ms, accs = [], []
    for i in range(2):
        if first:
            ms.append(jnp.full((rows, 1), -1e30, jnp.float32))
            accs.append(None)
        else:
            ms.append(m_in[i][:, :1])
            accs.append(acc_in[i])
    for start in range(0, keys, block_keys):
        kk = kv_ref[start : start + block_keys, :width]
        vv = vext[start : start + block_keys, :]
        for i in range(2):
            s = lax.dot_general(maps[i], kk, (((1,), (1,)), ((), ())), preferred_element_type=jnp.float32)
            m_new = jnp.maximum(ms[i], jnp.max(s, axis=1, keepdims=True))
            p = jnp.exp(s - m_new).astype(jnp.bfloat16)
            pv = jnp.dot(p, vv, preferred_element_type=jnp.float32)
            if accs[i] is None:
                accs[i] = pv
            else:
                accs[i] = accs[i] * jnp.exp(ms[i] - m_new) + pv
            ms[i] = m_new
    if last:
        o = [a[:, :vdim] / a[:, vdim:] for a in accs]
        differ = o[0] - lam_ref[0] * o[1]
        inverse = lax.rsqrt(jnp.mean(differ * differ, axis=1, keepdims=True) + EPSILON)
        out_ref[...] = (differ * inverse * gain_ref[...] * 0.8).astype(out_ref.dtype)
    else:
        for i in range(2):
            m_out[i] = jnp.broadcast_to(ms[i], (rows, m_out.shape[2]))
            acc_out[i] = accs[i]


def attend(lam, gain, q, kv, state, last, factor):
    rows, width = q.shape
    keys = kv.shape[0]
    vdim = kv.shape[1] - width
    block = min(256, rows)
    first = state is None
    smem = pl.BlockSpec(memory_space=pltpu.SMEM)
    m_spec = pl.BlockSpec((2, block, 128), lambda i: (0, i, 0))
    acc_spec = pl.BlockSpec((2, block, 2 * vdim), lambda i: (0, i, 0))
    in_specs = [
        smem,
        pl.BlockSpec((1, vdim), lambda i: (0, 0)),
        pl.BlockSpec((block, width), lambda i: (i, 0)),
        pl.BlockSpec((keys, width + vdim), lambda i: (0, 0)),
    ]
    args = [lam, gain, q, kv]
    aliases = {}
    if not first:
        in_specs += [m_spec, acc_spec]
        args += list(state)
        if not last:
            aliases = {4: 0, 5: 1}
    if last:
        out_shape = jax.ShapeDtypeStruct((rows, vdim), jnp.bfloat16)
        out_specs = pl.BlockSpec((block, vdim), lambda i: (i, 0))
    else:
        out_shape = (
            jax.ShapeDtypeStruct((2, rows, 128), jnp.float32),
            jax.ShapeDtypeStruct((2, rows, 2 * vdim), jnp.float32),
        )
        out_specs = (m_spec, acc_spec)
    return pl.pallas_call(
        functools.partial(attend_kernel, first, last, factor, min(1024, keys)),
        grid=(rows // block,),
        in_specs=in_specs,
        out_specs=out_specs,
        out_shape=out_shape,
        input_output_aliases=aliases,
        scratch_shapes=[pltpu.VMEM((keys, 2 * vdim), jnp.bfloat16)],
        compiler_params=pltpu.CompilerParams(dimension_semantics=("arbitrary",)),
    )(*args)


def layer_normed(heads_rows, residual_rows, out_weight, norm_gain):
    branch = jnp.dot(heads_rows, out_weight, preferred_element_type=jnp.float32)
    mixed_in = ALPHA * residual_rows.astype(jnp.float32) + branch
    row_mean = jnp.mean(mixed_in, axis=-1, keepdims=True)
    centered = mixed_in - row_mean
    row_var = jnp.mean(centered * centered, axis=-1, keepdims=True)
    return (centered * lax.rsqrt(row_var + EPSILON) * norm_gain).astype(jnp.bfloat16)


def on_device(
    stream,
    query_one,
    key_one,
    query_two,
    key_two,
    values,
    lambdas,
    head_gain,
    out_weight,
    norm_gain,
    gate_weight,
    up_weight,
    down_weight,
):
    heads = lambdas.shape[0]
    tokens = query_one.shape[0]
    head_width = query_one.shape[1] // heads
    vdim = values.shape[1] // heads
    hidden_units = gate_weight.shape[1]
    group = lax.axis_size("sp")
    tp = lax.axis_size("tp")
    ring = group // heads
    me = lax.axis_index("sp")
    factor = head_width ** (-0.5)

    half = hidden_units // 2
    x_bit, c_bit = lax.rem(me // 2, 2), lax.rem(me, 2)
    down_rows = down_weight.T
    halves = [
        jnp.concatenate([w[:, i * half : (i + 1) * half] for w in (gate_weight, up_weight, down_rows)], axis=1)
        for i in range(2)
    ]
    same, cross = [], []
    for d in range(group):
        base, x, c = d - d % 4, d // 2 % 2, d % 2
        same.append((d, base + 2 * c + x))
        cross.append((d, base + 2 * (1 - c) + x))
    got_same = lax.ppermute(jnp.where(c_bit == 0, halves[0], halves[1]), "sp", same)
    got_cross = lax.ppermute(jnp.where(c_bit == 0, halves[1], halves[0]), "sp", cross)
    packed = jnp.concatenate(
        [jnp.where(x_bit == 0, got_same, got_cross), jnp.where(x_bit == 0, got_cross, got_same)], axis=0
    )
    alike = [[d for d in range(group) if d // 2 % 2 == x] for x in range(2)]
    weights = lax.all_gather(packed, "sp", axis=0, axis_index_groups=alike, tiled=True)
    swap = [(d, d ^ 2) for d in range(group)]

    def by_head(a):
        return jnp.transpose(a.reshape(tokens, heads, a.shape[1] // heads), (1, 0, 2))

    own = jnp.concatenate([by_head(a) for a in (query_one, query_two, key_one, key_two, values)], axis=2)
    near = [[r * heads + h for h in range(heads)] for r in range(ring)]
    mine = lax.all_to_all(own, "sp", split_axis=0, concat_axis=0, axis_index_groups=near, tiled=True)
    mine = mine.reshape(heads * tokens, own.shape[2])
    q = mine[:, : 2 * head_width]
    kv = mine[:, 2 * head_width :]
    lam = lax.dynamic_slice_in_dim(lambdas, lax.rem(me, heads), 1, 0)
    gain = head_gain.reshape(1, vdim)
    onward = [(d, (d + heads) % group) for d in range(group)]
    state, other_stream = None, lax.ppermute(stream, "sp", swap)
    for step in range(ring):
        following = lax.ppermute(kv, "sp", onward) if step + 1 < ring else None
        state = attend(lam, gain, q, kv, state, step + 1 == ring, factor)
        if following is not None:
            state, kv, other_stream = lax.optimization_barrier((state, following, other_stream))
    back = lax.all_to_all(
        state.reshape(heads, tokens, vdim), "sp", split_axis=0, concat_axis=0, axis_index_groups=near, tiled=True
    )
    attended = jnp.transpose(back, (1, 0, 2)).reshape(tokens, heads * vdim)

    other_attended = lax.ppermute(attended, "sp", swap)

    def normed_of(rows, residual):
        by_rows = lax.all_to_all(rows, "tp", split_axis=0, concat_axis=1, tiled=True) if tp > 1 else rows
        normed = layer_normed(by_rows, residual, out_weight, norm_gain)
        return normed, (lax.all_gather(normed, "tp", axis=0, tiled=True) if tp > 1 else normed)

    def mixed(rows):
        gate_out = jnp.dot(rows, weights[:, :half], preferred_element_type=jnp.float32)
        upward = jnp.dot(rows, weights[:, half : 2 * half], preferred_element_type=jnp.float32)
        hidden = (jax.nn.silu(gate_out) * upward).astype(jnp.bfloat16)
        return lax.dot_general(
            hidden, weights[:, 2 * half :], (((1,), (1,)), ((), ())), preferred_element_type=jnp.float32
        )

    own_normed, own_all = normed_of(attended, stream)
    _, other_all = normed_of(other_attended, other_stream)
    from_other = lax.ppermute(mixed(other_all).astype(jnp.bfloat16), "sp", swap)
    partial_terms = lax.optimization_barrier(mixed(own_all)) + from_other.astype(jnp.float32)
    if tp > 1:
        partial_terms = lax.psum_scatter(
            partial_terms.astype(jnp.bfloat16), "tp", scatter_dimension=0, tiled=True
        ).astype(jnp.float32)
    return (ALPHA * own_normed.astype(jnp.float32) + 0.5 * partial_terms).astype(jnp.bfloat16)


def solution(mesh):
    return jax.shard_map(
        on_device,
        mesh=mesh,
        in_specs=(
            P(("sp", "tp"), None),
            P("sp", "tp"),
            P("sp", "tp"),
            P("sp", "tp"),
            P("sp", "tp"),
            P("sp", "tp"),
            P("tp"),
            P(),
            P(),
            P(),
            P("sp", "tp"),
            P("sp", "tp"),
            P("tp", "sp"),
        ),
        out_specs=P(("sp", "tp"), None),
        check_vma=False,
    )
```
